32 devices in a mesh: sp: 16 (over z, y, core), tp: 2 (over x).
Axes of the slice: x: 2, y: 2, z: 4, core: 2. Of those that a mesh axis runs over, the one named last changes fastest.
Arguments:
- latent_tokens: bfloat16 [2048, 2048], P(('sp', 'tp')), may hold values from -6 to 6
- context_tokens: bfloat16 [512, 2048], P('sp'), may hold values from -6 to 6
- cond: float32 [2048], replicated, may hold values from -6 to 6
- ctx_cond: float32 [2048], replicated, may hold values from -6 to 6
- mod_shift: bfloat16 [2048, 2048], P('sp', 'tp'), may hold values from -0.125 to 0.125
- mod_scale: bfloat16 [2048, 2048], P('sp', 'tp'), may hold values from -0.125 to 0.125
- mod_gate: bfloat16 [2048, 2048], P('sp', 'tp'), may hold values from -0.125 to 0.125
- norm_gain: float32 [2048], replicated, may hold values from 0.1 to 1.9
- w_query: bfloat16 [2048, 1536], P(None, 'tp'), may hold values from -0.125 to 0.125
- query_gain: float32 [96], replicated, may hold values from 0.8 to 2
- w_down_kv: bfloat16 [2048, 256], replicated, may hold values from -0.125 to 0.125
- w_rope_key: bfloat16 [2048, 32], replicated, may hold values from -0.125 to 0.125
- kv_gain: float32 [256], replicated, may hold values from 0.1 to 1.9
- w_up_kv: bfloat16 [2, 256, 1024], P(None, None, 'tp'), may hold values from -0.375 to 0.375
- key_gain: float32 [96], replicated, may hold values from 0.8 to 2
- ctx_lift: float32 [16], P('tp'), may hold values from 1.5 to 220
- w_output: bfloat16 [1024, 2048], P('tp'), may hold values from -0.1875 to 0.1875
Outputs:
- updated: bfloat16 [2048, 2048], P(('sp', 'tp'))
The draws below stay inside these ranges and needn't reach their ends.
All inputs are finite; a program needn't handle non-finite values.
Results may differ from the reference program's by a relative error of at most 0.007.
Values may be sent and summed in bfloat16 or wider, within the bound.
A program may use at most 64 MiB of HBM per device.

```python
import math
import jax
import jax.numpy as jnp
from jax import lax

D = 2048
HEADS = 16
HD = 64
ROPE = 32
KVL = 256
QK = 96
SEQ = 2048
CTX = 512
GRID_W = 64


def draw_ctx_lift(key, part):
    drawn = jax.random.uniform(jax.random.fold_in(key, 11), (HEADS,), jnp.float32, 1.5, 3.5)
    return drawn


def block_levels(rng, extent, split, smallest, high):
    gain = 1.0
    for dim, blocks in split:
        draws = jax.random.uniform(jax.random.fold_in(jax.random.fold_in(rng, 6), dim), (blocks,), jnp.float32, smallest / len(split), high / len(split))
        gain = gain * jnp.repeat(jnp.exp(draws), extent[dim] // blocks).reshape((-1,) + (1,) * (len(extent) - 1 - dim))
    return gain


def centred(stream_key, extent, deviation, reach, shards=(), held_as=jnp.bfloat16):
    array = jax.random.normal(stream_key, extent, jnp.float32) * deviation
    if len(shards) > 0:
        array = block_levels(stream_key, extent, shards, -0.22, 0.18) * array
    return jnp.clip(array, min=-reach, max=reach).astype(held_as)


def setup_inputs(seed: int = 0) -> dict:
    seeds = jax.random.split(jax.random.key(seed), 18)
    latent_tokens = centred(seeds[0], (SEQ, D), 1.0, 6.0, ((0, 32),))
    context_tokens = centred(seeds[1], (CTX, D), 1.0, 6.0, ((0, 16),))
    cond = centred(seeds[2], (D,), 1.0, 6.0, (), jnp.float32)
    ctx_cond = centred(seeds[3], (D,), 1.0, 6.0, (), jnp.float32)
    mod_shift = centred(seeds[4], (D, D), D ** -0.5, 0.125, ((0, 16), (1, 2)))
    mod_scale = centred(seeds[5], (D, D), D ** -0.5, 0.125, ((0, 16), (1, 2)))
    mod_gate = centred(seeds[6], (D, D), D ** -0.5, 0.125, ((0, 16), (1, 2)))
    norm_gain = jnp.clip(1.0 + 0.18 * jax.random.normal(seeds[7], (D,), jnp.float32), 0.1, 1.9)
    w_query = centred(seeds[8], (D, HEADS * QK), D ** -0.5, 0.125, ((1, 2),))
    query_gain = jnp.clip(jnp.exp(jax.random.uniform(seeds[9], (QK,), jnp.float32, math.log(0.8), math.log(2.0))), 0.8, 2.0)
    w_down_kv = centred(seeds[10], (D, KVL), D ** -0.5, 0.125)
    w_rope_key = centred(seeds[11], (D, ROPE), D ** -0.5, 0.125)
    kv_gain = jnp.clip(1.0 + 0.18 * jax.random.normal(seeds[12], (KVL,), jnp.float32), 0.1, 1.9)
    w_up_kv = centred(seeds[13], (2, KVL, HEADS * HD), KVL ** -0.5, 0.375, ((2, 2),))
    key_gain = jnp.clip(jnp.exp(jax.random.uniform(seeds[14], (QK,), jnp.float32, math.log(0.8), math.log(2.0))), 0.8, 2.0)
    ctx_lift = draw_ctx_lift(jax.random.fold_in(seeds[17], 71), 0)
    w_output = centred(seeds[16], (HEADS * HD, D), (HEADS * HD) ** -0.5, 0.1875, ((0, 2),))
    return dict(latent_tokens=latent_tokens, context_tokens=context_tokens, cond=cond, ctx_cond=ctx_cond, mod_shift=mod_shift, mod_scale=mod_scale, mod_gate=mod_gate, norm_gain=norm_gain, w_query=w_query, query_gain=query_gain, w_down_kv=w_down_kv, w_rope_key=w_rope_key, kv_gain=kv_gain, w_up_kv=w_up_kv, key_gain=key_gain, ctx_lift=ctx_lift, w_output=w_output)


EPS = 1e-06
THETA = 10000.0

def rms_normed(values, gain_vector):
    values = values.astype(jnp.float32)
    inv_root = lax.rsqrt(lax.optimization_barrier(jnp.mean(values * values, axis=-1, keepdims=True)) + EPS)
    return values * inv_root * gain_vector

def grid_angles(position, width):
    freq_count = width // 4
    inverse = THETA ** (-jnp.arange(freq_count, dtype=jnp.float32) / freq_count)
    row_index = (position // GRID_W).astype(jnp.float32)
    col_index = (position % GRID_W).astype(jnp.float32)
    return jnp.concatenate([row_index[:, None] * inverse, col_index[:, None] * inverse], axis=-1)

def rotate_tail(head_rows, angle, plain):
    tail = head_rows[..., plain:]
    half_width = tail.shape[-1] // 2
    cosine = jnp.cos(angle)[:, None, :]
    sine_val = jnp.sin(angle)[:, None, :]
    front_half = tail[..., :half_width]
    back_half = tail[..., half_width:]
    return jnp.concatenate([head_rows[..., :plain], front_half * cosine - back_half * sine_val, back_half * cosine + front_half * sine_val], axis=-1)

def modulation(signal, weight):
    return jnp.dot(signal, weight.astype(jnp.float32), precision=lax.Precision.HIGHEST)

def compress(hidden, w_down_kv, w_rope_key, kv_gain):
    latent = rms_normed(jnp.dot(hidden, w_down_kv, preferred_element_type=jnp.float32), kv_gain)
    rope_key = jnp.dot(hidden, w_rope_key, preferred_element_type=jnp.float32)
    return (latent.astype(jnp.bfloat16), rope_key.astype(jnp.bfloat16))

def expand(latent, rope_key, w_up_kv, key_gain, angle):
    row_count = latent.shape[0]
    head_count = w_up_kv.shape[2] // HD
    key_plain = jnp.dot(latent, w_up_kv[0], preferred_element_type=jnp.float32).reshape(row_count, head_count, HD)
    shared = jnp.broadcast_to(rope_key.astype(jnp.float32)[:, None, :], (row_count, head_count, ROPE))
    keys = rms_normed(jnp.concatenate([key_plain, shared], axis=-1), key_gain)
    if angle is not None:
        keys = rotate_tail(keys, angle, HD)
    values = jnp.dot(latent, w_up_kv[1], preferred_element_type=jnp.float32).astype(jnp.bfloat16)
    return (keys.astype(jnp.bfloat16), values.reshape(row_count, head_count, HD))

def reference(latent_tokens, context_tokens, cond, ctx_cond, mod_shift, mod_scale, mod_gate, norm_gain, w_query, query_gain, w_down_kv, w_rope_key, kv_gain, w_up_kv, key_gain, ctx_lift, w_output):
    lat_signal = jax.nn.silu(cond)
    ctx_signal = jax.nn.silu(ctx_cond)
    shift_lat = modulation(lat_signal, mod_shift)
    scale_lat = modulation(lat_signal, mod_scale)
    gate_lat = modulation(lat_signal, mod_gate)
    shift_ctx = modulation(ctx_signal, mod_shift)
    scale_ctx = modulation(ctx_signal, mod_scale)
    hidden_lat = (rms_normed(latent_tokens, norm_gain) * (1.0 + scale_lat) + shift_lat).astype(jnp.bfloat16)
    hidden_ctx = (rms_normed(context_tokens, norm_gain) * (1.0 + scale_ctx) + shift_ctx).astype(jnp.bfloat16)
    position = jnp.arange(SEQ, dtype=jnp.int32)
    angle = grid_angles(position, ROPE)
    queries = jnp.dot(hidden_lat, w_query, preferred_element_type=jnp.float32).reshape(SEQ, HEADS, QK)
    queries = rotate_tail(rms_normed(queries, query_gain), angle, HD).astype(jnp.bfloat16)
    lat_latent, lat_rope = compress(hidden_lat, w_down_kv, w_rope_key, kv_gain)
    ctx_latent, ctx_rope = compress(hidden_ctx, w_down_kv, w_rope_key, kv_gain)
    lat_keys, lat_values = expand(lat_latent, lat_rope, w_up_kv, key_gain, angle)
    ctx_keys, ctx_values = expand(ctx_latent, ctx_rope, w_up_kv, key_gain, None)
    all_keys = jnp.concatenate([ctx_keys, lat_keys], axis=0).astype(jnp.float32)
    all_values = jnp.concatenate([ctx_values, lat_values], axis=0).astype(jnp.float32)
    lift = jnp.concatenate([jnp.broadcast_to(ctx_lift[:, None], (HEADS, CTX)), jnp.zeros((HEADS, SEQ), jnp.float32)], axis=1)
    block = math.gcd(SEQ, 256)

    def attend(query_block):
        scores = jnp.einsum('qhd,khd->hqk', query_block.astype(jnp.float32), all_keys) * QK ** (-0.5)
        scores = scores + lift[:, None, :]
        highest = lax.optimization_barrier(jnp.max(scores, axis=-1, keepdims=True))
        weights = jnp.exp(scores - highest)
        total = lax.optimization_barrier(jnp.sum(weights, axis=-1))
        rounded = lax.optimization_barrier(weights.astype(jnp.bfloat16)).astype(jnp.float32)
        mixed = jnp.einsum('hqk,khd->qhd', rounded, all_values)
        return (mixed / jnp.transpose(total)[:, :, None]).astype(jnp.bfloat16)
    blocks = queries.reshape(SEQ // block, block, HEADS, QK)
    attended = lax.map(attend, blocks).reshape(SEQ, HEADS * HD)
    out = jnp.dot(attended, w_output, preferred_element_type=jnp.float32)
    return (latent_tokens.astype(jnp.float32) + gate_lat * out).astype(jnp.bfloat16)
```

```python
import functools

import jax
import jax.numpy as jnp
import numpy as np
from jax import lax
from jax.experimental import pallas as pl
from jax.experimental.pallas import tpu as pltpu
from jax.sharding import PartitionSpec as P

HD = 64
ROPE = 32
QK = 96
GRID_W = 64
EPS = 1e-06
THETA = 10000.0
LANE = 128
MESH = pl.DeviceIdType.MESH
F32 = jnp.float32
BF16 = jnp.bfloat16

NN = (((1,), (0,)), ((), ()))
NT = (((1,), (1,)), ((), ()))


def dot(a, b, dims=NN):
    return lax.dot_general(a, b, dims, preferred_element_type=F32)


def column(row):
    return jnp.transpose(jnp.broadcast_to(row, (LANE, row.shape[1])))


def kernel(
    sizes,
    tok_ref, ctx_ref, cond_ref, cctx_ref, mshift_ref, mscale_ref, mgate_ref, ngain_ref,
    wq_hbm, qgain_ref, wd_hbm, wr_hbm, kvgain_ref, wup_hbm, kgain_ref, lift_ref, wo_hbm,
    cos_ref, sin_ref,
    out_ref,
    wq, wd, wr, wup, wo, part, rsb, red, mod, tokall, hid, chid, G, H, X, rot, ssr, wkT, Q, att,
    sendb, recvb,
    wsem, tok_s, tok_r, rs_s, rs_r, ag_s, ag_r, gz_s, gz_r, hz_s, hz_r, gy_s, gy_r, hy_s, hy_r,
    gx_s, gx_r, gc_s, gc_r, hc_s, hc_r, ob_s, ob_r,
):
    SP, T, Y, C, q, rows, crows, heads = sizes
    Z = SP // (Y * C)
    ND = SP * T
    D = tok_ref.shape[1]
    group = rows * T
    crp = H.shape[3] - 16
    n_ctx = crows * SP
    n_lat = group * SP
    N = n_ctx + n_lat
    sp = lax.axis_index("sp")
    tp = lax.axis_index("tp")
    c = lax.rem(sp, C)
    y = lax.rem(sp // C, Y)
    z = sp // (C * Y)
    flat = sp * T + tp

    barrier = pltpu.get_barrier_semaphore()

    def greet(k, _):
        other = lax.rem(flat + k, ND)
        pl.semaphore_signal(barrier, inc=1, device_id=(other // T, lax.rem(other, T)), device_id_type=MESH)
        return 0

    lax.fori_loop(1, ND, greet, 0)

    wcopies = [
        pltpu.make_async_copy(src, dst, wsem.at[i])
        for i, (src, dst) in enumerate(((wq_hbm, wq), (wd_hbm, wd), (wr_hbm, wr), (wup_hbm, wup), (wo_hbm, wo)))
    ]
    for cp in wcopies:
        cp.start()

    sig_l = cond_ref[pl.ds(sp, 1), :]
    sig_l = column(sig_l * jax.nn.sigmoid(sig_l))
    sig_c = cctx_ref[pl.ds(sp, 1), :]
    sig_c = column(sig_c * jax.nn.sigmoid(sig_c))
    pcols = mshift_ref.shape[1] // LANE

    def put(v, j, val):
        i = v * pcols + j
        part[i // q, i % q : i % q + 1, :] = val

    for j in range(pcols):
        cols = slice(j * LANE, (j + 1) * LANE)
        w = mshift_ref[:, cols].astype(F32)
        put(0, j, jnp.sum(w * sig_l, axis=0, keepdims=True))
        put(1, j, jnp.sum(w * sig_c, axis=0, keepdims=True))
        w = mscale_ref[:, cols].astype(F32)
        put(2, j, jnp.sum(w * sig_l, axis=0, keepdims=True))
        put(3, j, jnp.sum(w * sig_c, axis=0, keepdims=True))
        w = mgate_ref[:, cols].astype(F32)
        put(4, j, jnp.sum(w * sig_l, axis=0, keepdims=True))
    for i in range(5 * pcols, SP * q):
        part[i // q, i % q : i % q + 1, :] = jnp.zeros((1, LANE), F32)

    pl.semaphore_wait(barrier, ND - 1)

    def rs_copy(k):
        other = lax.rem(sp + k, SP)
        return pltpu.make_async_remote_copy(
            src_ref=part.at[other], dst_ref=rsb.at[sp], send_sem=rs_s.at[k - 1], recv_sem=rs_r.at[k - 1],
            device_id=(other, tp), device_id_type=MESH)

    def rs_start(k, _):
        rs_copy(k).start()
        return 0

    lax.fori_loop(1, SP, rs_start, 0)

    def tp_copy(k, src, dst, s, r):
        return pltpu.make_async_remote_copy(
            src_ref=src, dst_ref=dst, send_sem=s.at[k - 1], recv_sem=r.at[k - 1],
            device_id=(sp, lax.rem(tp + k, T)), device_id_type=MESH)

    tok_copies = [tp_copy(k, tok_ref, tokall.at[tp], tok_s, tok_r) for k in range(1, T)]
    for cp in tok_copies:
        cp.start()

    rsb[sp] = part[sp]
    tokall[tp] = tok_ref[...]

    def rs_wait(k, _):
        rs_copy(k).wait()
        return 0

    lax.fori_loop(1, SP, rs_wait, 0)
    total = rsb[0]
    for i in range(1, SP):
        total = total + rsb[i]
    red[...] = total

    def ag_copy(k):
        other = lax.rem(flat + k, ND)
        return pltpu.make_async_remote_copy(
            src_ref=red, dst_ref=mod.at[tp, sp], send_sem=ag_s.at[k - 1], recv_sem=ag_r.at[k - 1],
            device_id=(other // T, lax.rem(other, T)), device_id_type=MESH)

    def ag_start(k, _):
        ag_copy(k).start()
        return 0

    lax.fori_loop(1, ND, ag_start, 0)
    mod[tp, sp] = total

    for cp in wcopies:
        cp.wait()
    wkT[...] = jnp.transpose(wup[0].astype(F32)).astype(BF16)
    kg = column(kgain_ref[...])
    qg = column(qgain_ref[...])
    for cp in tok_copies:
        cp.wait()
    xs = [tokall[t].astype(F32) for t in range(T)]
    invs = [lax.rsqrt(jnp.mean(x * x, axis=1, keepdims=True) + EPS) for x in xs]
    xc = ctx_ref[...].astype(F32)
    invc = lax.rsqrt(jnp.mean(xc * xc, axis=1, keepdims=True) + EPS)

    def ag_wait(k, _):
        ag_copy(k).wait()
        return 0

    lax.fori_loop(1, ND, ag_wait, 0)

    def vec(v, col):
        i = v * pcols + col % pcols
        return mod[col // pcols, i // q, i % q : i % q + 1, :]

    for j in range(D // LANE):
        cols = slice(j * LANE, (j + 1) * LANE)
        g = ngain_ref[:, cols]
        a, b = 1.0 + vec(2, j), vec(0, j)
        for t in range(T):
            hid[t, :, cols] = (tokall[t, :, cols].astype(F32) * invs[t] * g * a + b).astype(BF16)
        a, b = 1.0 + vec(3, j), vec(1, j)
        chid[:, cols] = (ctx_ref[:, cols].astype(F32) * invc * g * a + b).astype(BF16)

    def squeeze(h):
        raw = dot(h, wd[...])
        return raw * lax.rsqrt(jnp.mean(raw * raw, axis=1, keepdims=True) + EPS) * kvgain_ref[...]

    lane = lax.broadcasted_iota(jnp.int32, (ROPE, LANE), 1)
    H[z, y, c, 0:crows] = squeeze(chid[...]).astype(BF16)
    cr = dot(chid[...], wr[...])
    crt = jnp.transpose(jnp.concatenate([cr] * (LANE // crows), axis=0))
    clo = lax.rem(sp, LANE // crows) * crows
    crt = jnp.where((lane >= clo) & (lane < clo + crows), crt, 0.0).astype(BF16)
    H[z, y, c, crp : crp + 16] = jnp.concatenate([crt[:16], crt[16:]], axis=1)
    hid_all = hid[...].reshape(group, D)
    G[z, y, c, tp, 0:rows] = squeeze(hid[tp]).astype(BF16)
    lr = jnp.transpose(dot(hid_all, wr[...]))
    llo = tp * rows
    lr = jnp.where((lane >= llo) & (lane < llo + rows), lr, 0.0).astype(BF16)
    G[z, y, c, tp, rows : rows + 16] = jnp.concatenate([lr[:16], lr[16:]], axis=1)

    def at(zz, yy, cc):
        return (zz * Y + yy) * C + cc

    def remote(src, s, r, dev):
        return pltpu.make_async_remote_copy(
            src_ref=src, dst_ref=src, send_sem=s, recv_sem=r, device_id=dev, device_id_type=MESH)

    zc = []
    for k in range(1, Z):
        dev = (at(lax.rem(z + k, Z), y, c), tp)
        zc.append(remote(G.at[z, y, c, tp], gz_s.at[k - 1], gz_r.at[k - 1], dev))
        zc.append(remote(H.at[z, y, c], hz_s.at[k - 1], hz_r.at[k - 1], dev))
    for cp in zc:
        cp.start()

    raw = dot(hid_all, wq[...])
    rawT = jnp.transpose(raw)
    cosg = cos_ref[:, pl.ds(pl.multiple_of(sp * group, group), group)]
    sing = sin_ref[:, pl.ds(pl.multiple_of(sp * group, group), group)]
    fold = QK ** (-0.5) * 1.4426950408889634
    for h in range(heads):
        u = rawT[h * QK : (h + 1) * QK]
        u = u * (lax.rsqrt(jnp.mean(u * u, axis=0, keepdims=True) + EPS) * fold) * qg[:, :group]
        f, b = u[HD : HD + 16], u[HD + 16 :]
        u = jnp.concatenate([u[:HD], f * cosg - b * sing, b * cosg + f * sing], axis=0)
        Q[h] = jnp.transpose(u).astype(BF16)

    for cp in zc:
        cp.wait()

    ydev = (at(z, Y - 1 - y, c), tp)

    def both(copies):
        for cp in copies:
            cp.start()
        for cp in copies:
            cp.wait()

    def xdev(k):
        return (sp, lax.rem(tp + k, T))

    @pl.when(c == 0)
    def _():
        both([
            remote(G.at[:, y, 0, tp], gy_s.at[0], gy_r.at[0], ydev),
            remote(H.at[:, y, 0], hy_s.at[0], hy_r.at[0], ydev),
        ])
        both([remote(G.at[:, :, 0, tp], gx_s.at[k - 1], gx_r.at[k - 1], xdev(k)) for k in range(1, T)])

    @pl.when(c != 0)
    def _():
        both([remote(G.at[:, y, 1, tp], gx_s.at[k - 1], gx_r.at[k - 1], xdev(k)) for k in range(1, T)])
        both([
            remote(G.at[:, y, 1], gy_s.at[0], gy_r.at[0], ydev),
            remote(H.at[:, y, 1], hy_s.at[0], hy_r.at[0], ydev),
        ])

    cdev = (at(z, y, C - 1 - c), tp)
    both([
        remote(G.at[:, :, c], gc_s.at[0], gc_r.at[0], cdev),
        remote(H.at[:, :, c], hc_s.at[0], hc_r.at[0], cdev),
    ])

    def where_is(s):
        return s // (Y * C), (s // C) % Y, s % C

    step = crows if crows % 16 == 0 else 16
    if crows % 16 == 0:
        for s in range(SP):
            zz, yy, cc = where_is(s)
            X[s * crows : (s + 1) * crows] = H[zz, yy, cc, 0:crows]
    else:
        X[0:n_ctx] = jnp.concatenate(
            [H[where_is(s)][0:16].astype(F32)[:crows] for s in range(SP)], axis=0).astype(BF16)
    per = LANE // crows
    gk = kg[HD:]
    gf, gb = gk[:16], gk[16:]
    for s0 in range(0, SP, per):
        both_half = sum(H[where_is(s)][crp : crp + 16].astype(F32) for s in range(s0, s0 + per))
        f, b = both_half[:, :LANE], both_half[:, LANE:]
        cols = slice(s0 * crows, s0 * crows + LANE)
        ssr[:, cols] = jnp.sum(f * f + b * b, axis=0, keepdims=True)
        rot[0:16, cols] = f * gf
        rot[16:32, cols] = b * gb
    for s in range(SP):
        zz, yy, cc = where_is(s)
        total = 0.0
        for t in range(T):
            lo = n_ctx + s * group + t * rows
            X[lo : lo + rows] = G[zz, yy, cc, t, 0:rows]
            total = total + G[zz, yy, cc, t, rows : rows + 16].astype(F32)
        f, b = total[:, :LANE], total[:, LANE:]
        cols = slice(n_ctx + s * group, n_ctx + (s + 1) * group)
        pos = slice(s * group, (s + 1) * group)
        ssr[:, cols] = jnp.sum(f * f + b * b, axis=0, keepdims=True)
        f, b = f * gf, b * gb
        rot[0:16, cols] = f * cos_ref[:, pos] - b * sin_ref[:, pos]
        rot[16:32, cols] = b * cos_ref[:, pos] + f * sin_ref[:, pos]

    gp = kg[:HD, :1]
    ones = jnp.ones((N, LANE), BF16)
    half = lax.broadcasted_iota(jnp.int32, (group, LANE), 1) < HD

    def pair(p, _):
        lo = pl.multiple_of(p * LANE, LANE)
        kT = dot(wkT[pl.ds(lo, LANE), :], X[...], NT)
        val = jnp.concatenate([dot(X[...], wup[1, :, pl.ds(lo, LANE)]).astype(BF16), ones], axis=1)
        res = []
        for i in range(2):
            kp = kT[i * HD : (i + 1) * HD]
            inv = lax.rsqrt((jnp.sum(kp * kp, axis=0, keepdims=True) + ssr[...]) * (1.0 / QK) + EPS)
            key = jnp.concatenate([kp * gp * inv, rot[...] * inv], axis=0).astype(BF16)
            w = jnp.exp2(dot(Q[2 * p + i], key)).astype(BF16)
            drop = jnp.exp(jnp.full((1, 2 * LANE), -lift_ref[2 * p + i], F32))
            o = dot(w[:, :n_ctx], val[:n_ctx]) + drop * dot(w[:, n_ctx:], val[n_ctx:])
            res.append(o[:, :LANE] / o[:, LANE:])
        att[:, pl.ds(lo, LANE)] = jnp.where(half, res[0], res[1]).astype(BF16)
        return 0

    lax.fori_loop(0, heads // 2, pair, 0)

    for k in range(1, T):
        t = lax.rem(tp + k, T)
        a = att[pl.ds(pl.multiple_of(t * rows, rows), rows), :]
        sendb[k - 1] = dot(a, wo[...]).astype(BF16)
    copies = [tp_copy(k, sendb.at[k - 1], recvb.at[k - 1], ob_s, ob_r) for k in range(1, T)]
    for cp in copies:
        cp.start()
    acc = dot(att[pl.ds(pl.multiple_of(tp * rows, rows), rows), :], wo[...])
    for cp in copies:
        cp.wait()
    for k in range(1, T):
        acc = acc + recvb[k - 1].astype(F32)
    for j in range(D // LANE):
        cols = slice(j * LANE, (j + 1) * LANE)
        out_ref[:, cols] = (tok_ref[:, cols].astype(F32) + vec(4, j) * acc[:, cols]).astype(BF16)


def local(
    latent_tokens, context_tokens, cond, ctx_cond, mod_shift, mod_scale, mod_gate, norm_gain,
    w_query, query_gain, w_down_kv, w_rope_key, kv_gain, w_up_kv, key_gain, ctx_lift, w_output,
):
    SP, T = lax.axis_size("sp"), lax.axis_size("tp")
    Y = C = 2
    Z = SP // (Y * C)
    rows, D = latent_tokens.shape
    crows = context_tokens.shape[0]
    heads = ctx_lift.shape[0]
    prows, pcols = mod_shift.shape
    kvl = w_down_kv.shape[1]
    q = -(-(5 * pcols // LANE) // SP)
    group = rows * T
    seq = group * SP
    n = seq + crows * SP
    crp = max(16, crows)
    inv = THETA ** (-np.arange(ROPE // 4, dtype=np.float64) / (ROPE // 4))
    pos = np.arange(seq)
    ang = np.concatenate([inv[:, None] * (pos // GRID_W), inv[:, None] * (pos % GRID_W)], axis=0)
    cos, sin = np.cos(ang).astype(np.float32), np.sin(ang).astype(np.float32)
    vm = pl.BlockSpec(memory_space=pltpu.VMEM)
    hbm = pl.BlockSpec(memory_space=pl.ANY)
    sm = pl.BlockSpec(memory_space=pltpu.SMEM)
    dma = pltpu.SemaphoreType.DMA
    V = pltpu.VMEM
    ND = SP * T
    return pl.pallas_call(
        functools.partial(kernel, (SP, T, Y, C, q, rows, crows, heads)),
        out_shape=jax.ShapeDtypeStruct((rows, D), BF16),
        in_specs=[vm] * 8 + [hbm, vm, hbm, hbm, vm, hbm, vm, sm, hbm, vm, vm],
        out_specs=vm,
        scratch_shapes=[
            V(w_query.shape, BF16), V(w_down_kv.shape, BF16), V(w_rope_key.shape, BF16),
            V(w_up_kv.shape, BF16), V(w_output.shape, BF16),
            V((SP, q, LANE), F32), V((SP, q, LANE), F32), V((q, LANE), F32), V((T, SP, q, LANE), F32),
            V((T, rows, D), BF16), V((T, rows, D), BF16), V((crows, D), BF16),
            V((Z, Y, C, T, rows + 16, kvl), BF16), V((Z, Y, C, crp + 16, kvl), BF16),
            V((n, kvl), BF16), V((ROPE, n), F32), V((1, n), F32), V((w_up_kv.shape[2], kvl), BF16),
            V((heads, group, QK), BF16), V((group, heads * HD), BF16),
            V((T - 1, rows, D), BF16), V((T - 1, rows, D), BF16),
            dma((5,)), dma((T - 1,)), dma((T - 1,)), dma((SP - 1,)), dma((SP - 1,)),
            dma((ND - 1,)), dma((ND - 1,)), dma((Z - 1,)), dma((Z - 1,)), dma((Z - 1,)), dma((Z - 1,)),
            dma((1,)), dma((1,)), dma((1,)), dma((1,)), dma((T - 1,)), dma((T - 1,)),
            dma((1,)), dma((1,)), dma((1,)), dma((1,)), dma((T - 1,)), dma((T - 1,)),
        ],
        compiler_params=pltpu.CompilerParams(
            collective_id=0, has_side_effects=True, vmem_limit_bytes=60 * 1024 * 1024),
    )(
        latent_tokens, context_tokens, cond.reshape(SP, prows), ctx_cond.reshape(SP, prows),
        mod_shift, mod_scale, mod_gate, norm_gain.reshape(1, -1), w_query, query_gain.reshape(1, -1),
        w_down_kv, w_rope_key, kv_gain.reshape(1, -1), w_up_kv, key_gain.reshape(1, -1), ctx_lift,
        w_output, cos, sin,
    )


def solution(mesh):
    return jax.shard_map(
        local,
        mesh=mesh,
        in_specs=(
            P(("sp", "tp"), None),
            P("sp", None),
            P(),
            P(),
            P("sp", "tp"),
            P("sp", "tp"),
            P("sp", "tp"),
            P(),
            P(None, "tp"),
            P(),
            P(),
            P(),
            P(),
            P(None, None, "tp"),
            P(),
            P("tp"),
            P("tp", None),
        ),
        out_specs=P(("sp", "tp"), None),
        check_vma=False,
    )
```

```python
import functools

import jax
import jax.numpy as jnp
import numpy as np
from jax import lax
from jax.experimental import pallas as pl
from jax.experimental.pallas import tpu as pltpu
from jax.sharding import PartitionSpec as P

HD = 64
ROPE = 32
QK = 96
GRID_W = 64
EPS = 1e-06
THETA = 10000.0
LANE = 128
MESH = pl.DeviceIdType.MESH
F32 = jnp.float32
BF16 = jnp.bfloat16

NN = (((1,), (0,)), ((), ()))
NT = (((1,), (1,)), ((), ()))


def dot(a, b, dims=NN):
    return lax.dot_general(a, b, dims, preferred_element_type=F32)


def column(row):
    return jnp.transpose(jnp.broadcast_to(row, (LANE, row.shape[1])))


def kernel(
    sizes,
    tok_ref, ctx_ref, cond_ref, cctx_ref, mshift_hbm, mscale_hbm, mgate_hbm, ngain_ref,
    wq_hbm, qgain_ref, wd_hbm, wr_hbm, kvgain_ref, wup_hbm, kgain_ref, lift_ref, wo_hbm,
    cos_hbm, sin_hbm,
    out_hbm,
    mshift_ref, mscale_ref, mgate_ref, cos_ref, sin_ref, out_ref,
    wq, wd, wr, wup, wo, part, rsb, red, mod, tokall, hid, chid, G, H, X, rot, ssr, wkT, Q, att,
    sendb, recvb,
    wsem, osem, tok_s, tok_r, rs_s, rs_r, ag_s, ag_r, gz_s, gz_r, hz_s, hz_r, gy_s, gy_r, hy_s, hy_r,
    gx_s, gx_r, gc_s, gc_r, hc_s, hc_r, f2_s, f2_r, f3_s, f3_r, ob_s, ob_r,
):
    SP, T, Y, C, q, rows, crows, heads, split, chunks = sizes
    Z = SP // (Y * C)
    ND = SP * T
    D = tok_ref.shape[1]
    group = rows * T
    crp = H.shape[3] - 16
    n_ctx = crows * SP
    n_lat = group * SP
    N = n_ctx + n_lat
    sp = lax.axis_index("sp")
    tp = lax.axis_index("tp")
    c = lax.rem(sp, C)
    y = lax.rem(sp // C, Y)
    z = sp // (C * Y)
    flat = sp * T + tp

    barrier = pltpu.get_barrier_semaphore()

    def greet(k, _):
        other = lax.rem(flat + k, ND)
        pl.semaphore_signal(barrier, inc=1, device_id=(other // T, lax.rem(other, T)), device_id_type=MESH)
        return 0

    lax.fori_loop(1, ND, greet, 0)

    wcopies = [
        pltpu.make_async_copy(src, dst, wsem.at[i])
        for i, (src, dst) in enumerate((
            (mshift_hbm, mshift_ref), (mscale_hbm, mscale_ref), (mgate_hbm, mgate_ref), (wd_hbm, wd),
            (wr_hbm, wr), (wup_hbm, wup), (cos_hbm, cos_ref), (sin_hbm, sin_ref), (wq_hbm, wq), (wo_hbm, wo)))
    ]
    for cp in wcopies:
        cp.start()

    sig_l = cond_ref[pl.ds(sp, 1), :]
    sig_l = column(sig_l * jax.nn.sigmoid(sig_l))
    sig_c = cctx_ref[pl.ds(sp, 1), :]
    sig_c = column(sig_c * jax.nn.sigmoid(sig_c))
    pcols = mshift_ref.shape[1] // LANE
    for cp in wcopies[:3]:
        cp.wait()

    def put(v, j, val):
        i = v * pcols + j
        part[i // q, i % q : i % q + 1, :] = val

    for j in range(pcols):
        cols = slice(j * LANE, (j + 1) * LANE)
        w = mshift_ref[:, cols].astype(F32)
        put(0, j, jnp.sum(w * sig_l, axis=0, keepdims=True))
        put(1, j, jnp.sum(w * sig_c, axis=0, keepdims=True))
        w = mscale_ref[:, cols].astype(F32)
        put(2, j, jnp.sum(w * sig_l, axis=0, keepdims=True))
        put(3, j, jnp.sum(w * sig_c, axis=0, keepdims=True))
        w = mgate_ref[:, cols].astype(F32)
        put(4, j, jnp.sum(w * sig_l, axis=0, keepdims=True))
    for i in range(5 * pcols, SP * q):
        part[i // q, i % q : i % q + 1, :] = jnp.zeros((1, LANE), F32)

    pl.semaphore_wait(barrier, ND - 1)

    def rs_copy(k):
        other = lax.rem(sp + k, SP)
        return pltpu.make_async_remote_copy(
            src_ref=part.at[other], dst_ref=rsb.at[sp], send_sem=rs_s.at[k - 1], recv_sem=rs_r.at[k - 1],
            device_id=(other, tp), device_id_type=MESH)

    def rs_start(k, _):
        rs_copy(k).start()
        return 0

    lax.fori_loop(1, SP, rs_start, 0)

    def tp_copy(k, src, dst, s, r):
        return pltpu.make_async_remote_copy(
            src_ref=src, dst_ref=dst, send_sem=s.at[k - 1], recv_sem=r.at[k - 1],
            device_id=(sp, lax.rem(tp + k, T)), device_id_type=MESH)

    tok_copies = [tp_copy(k, tok_ref, tokall.at[tp], tok_s, tok_r) for k in range(1, T)]
    rsb[sp] = part[sp]

    def rs_wait(k, _):
        rs_copy(k).wait()
        return 0

    lax.fori_loop(1, SP, rs_wait, 0)
    total = rsb[0]
    for i in range(1, SP):
        total = total + rsb[i]
    red[...] = total

    def ag_copy(k):
        other = lax.rem(flat + k, ND)
        return pltpu.make_async_remote_copy(
            src_ref=red, dst_ref=mod.at[tp, sp], send_sem=ag_s.at[k - 1], recv_sem=ag_r.at[k - 1],
            device_id=(other // T, lax.rem(other, T)), device_id_type=MESH)

    def ag_start(k, _):
        ag_copy(k).start()
        return 0

    lax.fori_loop(1, ND, ag_start, 0)
    for cp in tok_copies:
        cp.start()
    mod[tp, sp] = total

    for cp in wcopies[3:6]:
        cp.wait()
    wkT[...] = jnp.transpose(wup[0].astype(F32)).astype(BF16)
    kg = column(kgain_ref[...])
    qg = column(qgain_ref[...])
    my_ctx = ctx_ref[pl.ds(pl.multiple_of(tp * 16, 16), 16), :] if split else ctx_ref[...]
    my_ctx = my_ctx.astype(F32)
    invc = lax.rsqrt(jnp.mean(my_ctx * my_ctx, axis=1, keepdims=True) + EPS)
    my_tok = tok_ref[...].astype(F32)
    invt = lax.rsqrt(jnp.mean(my_tok * my_tok, axis=1, keepdims=True) + EPS)

    def ag_wait(k, _):
        ag_copy(k).wait()
        return 0

    lax.fori_loop(1, ND, ag_wait, 0)

    def vec(v, col):
        i = v * pcols + col % pcols
        return mod[col // pcols, i // q, i % q : i % q + 1, :]

    def modulate(x, inv, j, a, b):
        cols = slice(j * LANE, (j + 1) * LANE)
        return (x[:, cols] * inv * ngain_ref[:, cols] * (1.0 + vec(a, j)) + vec(b, j)).astype(BF16)

    for j in range(D // LANE):
        cols = slice(j * LANE, (j + 1) * LANE)
        hid[tp, :, cols] = modulate(my_tok, invt, j, 2, 0)
        chid[:, cols] = modulate(my_ctx, invc, j, 3, 1)

    def squeeze(raw):
        return (raw * lax.rsqrt(jnp.mean(raw * raw, axis=1, keepdims=True) + EPS) * kvgain_ref[...]).astype(BF16)

    lane = lax.broadcasted_iota(jnp.int32, (ROPE, LANE), 1)
    own = hid[tp]
    own_c = chid[...]
    crn = own_c.shape[0]
    lrope = dot(wr[...], jnp.concatenate([own] * T, axis=0), NT)
    crope = dot(wr[...], jnp.concatenate([own_c.astype(F32)] * (LANE // crn), axis=0).astype(BF16), NT)
    llo = tp * rows
    lrope = jnp.where((lane >= llo) & (lane < llo + rows), lrope, 0.0)
    per = (rows if split else LANE) // crn
    clo = lax.rem(sp, per) * crn
    if split:
        clo = clo + lax.rem(tp + 1, T) * rows
    crope = jnp.where((lane >= clo) & (lane < clo + crn), crope, 0.0)
    if split:
        lrope = lrope + crope
        lats = squeeze(dot(jnp.concatenate([own, own_c], axis=0), wd[...]))
        G[z, y, c, tp, rows + 16 : rows + 32] = lats[rows:]
        G[z, y, c, tp, 0:rows] = lats[:rows]
    else:
        H[z, y, c, 0:crows] = squeeze(dot(own_c, wd[...]))
        H[z, y, c, crp : crp + 16] = jnp.concatenate([crope[:16], crope[16:]], axis=1).astype(BF16)
        G[z, y, c, tp, 0:rows] = squeeze(dot(own, wd[...]))
    G[z, y, c, tp, rows : rows + 16] = jnp.concatenate([lrope[:16], lrope[16:]], axis=1).astype(BF16)

    def at(zz, yy, cc):
        return (zz * Y + yy) * C + cc

    def remote(src, s, r, dev):
        return pltpu.make_async_remote_copy(
            src_ref=src, dst_ref=src, send_sem=s, recv_sem=r, device_id=dev, device_id_type=MESH)

    zc = []
    for k in range(1, Z):
        dev = (at(lax.rem(z + k, Z), y, c), tp)
        zc.append(remote(G.at[z, y, c, tp], gz_s.at[k - 1], gz_r.at[k - 1], dev))
        if not split:
            zc.append(remote(H.at[z, y, c], hz_s.at[k - 1], hz_r.at[k - 1], dev))
    for cp in zc:
        cp.start()

    for cp in tok_copies:
        cp.wait()
    for k in range(1, T):
        t = lax.rem(tp + k, T)
        x = tokall[t].astype(F32)
        inv = lax.rsqrt(jnp.mean(x * x, axis=1, keepdims=True) + EPS)
        for j in range(D // LANE):
            hid[t, :, j * LANE : (j + 1) * LANE] = modulate(x, inv, j, 2, 0)
    for cp in wcopies[6:9]:
        cp.wait()
    hid_all = hid[...].reshape(group, D)
    raw = dot(hid_all, wq[...])
    rawT = jnp.transpose(raw)
    cosg = cos_ref[:, pl.ds(pl.multiple_of(sp * group, group), group)]
    sing = sin_ref[:, pl.ds(pl.multiple_of(sp * group, group), group)]
    fold = QK ** (-0.5) * 1.4426950408889634
    for h in range(heads):
        u = rawT[h * QK : (h + 1) * QK]
        u = u * (lax.rsqrt(jnp.mean(u * u, axis=0, keepdims=True) + EPS) * fold) * qg[:, :group]
        f, b = u[HD : HD + 16], u[HD + 16 :]
        u = jnp.concatenate([u[:HD], f * cosg - b * sing, b * cosg + f * sing], axis=0)
        Q[h] = jnp.transpose(u).astype(BF16)

    for cp in zc:
        cp.wait()

    ydev = (at(z, Y - 1 - y, c), tp)
    cdev = (at(z, y, C - 1 - c), tp)

    def xdev(k):
        return (sp, lax.rem(tp + k, T))

    def start(copies):
        for cp in copies:
            cp.start()
        return copies

    def wait(copies):
        for cp in copies:
            cp.wait()

    def finish(sent, got):
        for cp in sent:
            cp.wait_send()
        for cp in got:
            cp.wait_recv()

    first = start([remote(G.at[:, y, c, tp], gc_s.at[0], gc_r.at[0], cdev)])
    others = [lax.rem(tp + k, T) for k in range(1, T)]

    def fwd2(cc):
        if cc == 0:
            return [remote(G.at[:, 1 - y, 0, tp], f2_s.at[0], f2_r.at[0], cdev)]
        return [remote(G.at[:, y, 1, t], f2_s.at[k], f2_r.at[k], cdev) for k, t in enumerate(others)]

    def fwd3(cc):
        if cc == 0:
            return [remote(G.at[:, :, 0, t], f3_s.at[k], f3_r.at[k], cdev) for k, t in enumerate(others)]
        return [remote(G.at[:, 1 - y, 1], f3_s.at[0], f3_r.at[0], cdev)]

    @pl.when(c == 0)
    def _():
        wait(start([remote(G.at[:, y, 0, tp], gy_s.at[0], gy_r.at[0], ydev)]))
        last = start([remote(G.at[:, :, 0, tp], gx_s.at[k - 1], gx_r.at[k - 1], xdev(k)) for k in range(1, T)])
        sent = start(fwd2(0))
        wait(last)
        finish(sent + start(fwd3(0)), fwd2(1) + fwd3(1))

    @pl.when(c != 0)
    def _():
        wait(start([remote(G.at[:, y, 1, tp], gx_s.at[k - 1], gx_r.at[k - 1], xdev(k)) for k in range(1, T)]))
        last = start([remote(G.at[:, y, 1], gy_s.at[0], gy_r.at[0], ydev)])
        sent = start(fwd2(1))
        wait(last)
        finish(sent + start(fwd3(1)), fwd2(0) + fwd3(0))

    wait(first)
    if not split:
        wait(start([remote(H.at[:, y, c], hy_s.at[0], hy_r.at[0], ydev)]))
        wait(start([remote(H.at[:, :, c], hc_s.at[0], hc_r.at[0], cdev)]))

    def where_is(s):
        return s // (Y * C), (s // C) % Y, s % C

    gk = kg[HD:]
    gf, gb = gk[:16], gk[16:]

    def place(cols, total, pos):
        f, b = total[:, :LANE], total[:, LANE:]
        ssr[:, cols] = jnp.sum(f * f + b * b, axis=0, keepdims=True)
        f, b = f * gf, b * gb
        if pos is not None:
            cs, sn = cos_ref[:, pos], sin_ref[:, pos]
            f, b = f * cs - b * sn, b * cs + f * sn
        rot[0:16, cols] = f
        rot[16:32, cols] = b

    lane2 = lax.rem(lax.broadcasted_iota(jnp.int32, (16, 2 * LANE), 1), LANE) // rows

    def mix(blocks):
        total = blocks[0]
        for t in range(1, T):
            total = jnp.where(lane2 == t, blocks[t], total)
        return total

    ctotal = 0.0
    for s in range(SP):
        w = where_is(s)
        lo = n_ctx + s * group
        for t in range(T):
            X[lo + t * rows : lo + (t + 1) * rows] = G[w[0], w[1], w[2], t, 0:rows]
        blocks = [G[w[0], w[1], w[2], t, rows : rows + 16].astype(F32) for t in range(T)]
        place(slice(lo, lo + group), mix(blocks), slice(s * group, (s + 1) * group))
        if split:
            base = s // per * group
            for t in range(T):
                lo = base + (t + 1) % T * rows + s % per * 16
                X[lo : lo + 16] = G[w[0], w[1], w[2], t, rows + 16 : rows + 32]
            ctotal = ctotal + mix([blocks[(t - 1) % T] for t in range(T)])
            if s % per == per - 1:
                place(slice(base, base + group), ctotal, None)
                ctotal = 0.0
    if not split:
        if crows % 16 == 0:
            for s in range(SP):
                w = where_is(s)
                X[s * crows : (s + 1) * crows] = H[w[0], w[1], w[2], 0:crows]
        else:
            X[0:n_ctx] = jnp.concatenate(
                [H[where_is(s)][0:16].astype(F32)[:crows] for s in range(SP)], axis=0).astype(BF16)
        for s0 in range(0, SP, per):
            total = sum(H[where_is(s)][crp : crp + 16].astype(F32) for s in range(s0, s0 + per))
            place(slice(s0 * crows, s0 * crows + LANE), total, None)

    gp = kg[:HD, :1]
    ones = jnp.ones((N, LANE), BF16)
    half = lax.broadcasted_iota(jnp.int32, (group, LANE), 1) < HD

    def pair(p, _):
        lo = pl.multiple_of(p * LANE, LANE)
        kT = dot(wkT[pl.ds(lo, LANE), :], X[...], NT)
        val = jnp.concatenate([dot(X[...], wup[1, :, pl.ds(lo, LANE)]).astype(BF16), ones], axis=1)
        res = []
        for i in range(2):
            kp = kT[i * HD : (i + 1) * HD]
            inv = lax.rsqrt((jnp.sum(kp * kp, axis=0, keepdims=True) + ssr[...]) * (1.0 / QK) + EPS)
            key = jnp.concatenate([kp * gp * inv, rot[...] * inv], axis=0).astype(BF16)
            w = jnp.exp2(dot(Q[2 * p + i], key)).astype(BF16)
            drop = jnp.exp(jnp.full((1, 2 * LANE), -lift_ref[2 * p + i], F32))
            o = dot(w[:, :n_ctx], val[:n_ctx]) + drop * dot(w[:, n_ctx:], val[n_ctx:])
            res.append(o[:, :LANE] / o[:, LANE:])
        att[:, pl.ds(lo, LANE)] = jnp.where(half, res[0], res[1]).astype(BF16)
        return 0

    lax.fori_loop(0, heads // 2, pair, 0)

    wcopies[9].wait()
    width = D // chunks
    copies = []
    for j in range(chunks):
        cols = slice(j * width, (j + 1) * width)
        for k in range(1, T):
            t = lax.rem(tp + k, T)
            a = att[pl.ds(pl.multiple_of(t * rows, rows), rows), :]
            sendb[k - 1, :, cols] = dot(a, wo[:, cols]).astype(BF16)
            cp = pltpu.make_async_remote_copy(
                src_ref=sendb.at[k - 1, :, cols], dst_ref=recvb.at[k - 1, :, cols],
                send_sem=ob_s.at[j, k - 1], recv_sem=ob_r.at[j, k - 1],
                device_id=xdev(k), device_id_type=MESH)
            cp.start()
            copies.append(cp)
    acc = dot(att[pl.ds(pl.multiple_of(tp * rows, rows), rows), :], wo[...])
    outs = []
    for j in range(chunks):
        for k in range(1, T):
            copies[j * (T - 1) + k - 1].wait()
        for i in range(j * width // LANE, (j + 1) * width // LANE):
            cols = slice(i * LANE, (i + 1) * LANE)
            o = acc[:, cols]
            for k in range(1, T):
                o = o + recvb[k - 1, :, cols].astype(F32)
            out_ref[:, cols] = (tok_ref[:, cols].astype(F32) + vec(4, i) * o).astype(BF16)
        cols = slice(j * width, (j + 1) * width)
        cp = pltpu.make_async_copy(out_ref.at[:, cols], out_hbm.at[:, cols], osem.at[j])
        cp.start()
        outs.append(cp)
    for cp in outs:
        cp.wait()


def local(
    latent_tokens, context_tokens, cond, ctx_cond, mod_shift, mod_scale, mod_gate, norm_gain,
    w_query, query_gain, w_down_kv, w_rope_key, kv_gain, w_up_kv, key_gain, ctx_lift, w_output,
):
    SP, T = lax.axis_size("sp"), lax.axis_size("tp")
    Y = C = 2
    Z = SP // (Y * C)
    rows, D = latent_tokens.shape
    crows = context_tokens.shape[0]
    heads = ctx_lift.shape[0]
    prows, pcols = mod_shift.shape
    kvl = w_down_kv.shape[1]
    q = -(-(5 * pcols // LANE) // SP)
    group = rows * T
    seq = group * SP
    n = seq + crows * SP
    split = crows == 16 * T
    crp = 16 if split else max(16, crows)
    chunks = 4
    inv = THETA ** (-np.arange(ROPE // 4, dtype=np.float64) / (ROPE // 4))
    pos = np.arange(seq)
    ang = np.concatenate([inv[:, None] * (pos // GRID_W), inv[:, None] * (pos % GRID_W)], axis=0)
    cos, sin = np.cos(ang).astype(np.float32), np.sin(ang).astype(np.float32)
    vm = pl.BlockSpec(memory_space=pltpu.VMEM)
    hbm = pl.BlockSpec(memory_space=pl.ANY)
    sm = pl.BlockSpec(memory_space=pltpu.SMEM)
    dma = pltpu.SemaphoreType.DMA
    V = pltpu.VMEM
    ND = SP * T
    return pl.pallas_call(
        functools.partial(kernel, (SP, T, Y, C, q, rows, crows, heads, split, chunks)),
        out_shape=jax.ShapeDtypeStruct((rows, D), BF16),
        in_specs=[vm] * 4 + [hbm] * 3 + [vm, hbm, vm, hbm, hbm, vm, hbm, vm, sm, hbm, hbm, hbm],
        out_specs=hbm,
        scratch_shapes=[
            V(mod_shift.shape, BF16), V(mod_shift.shape, BF16), V(mod_shift.shape, BF16),
            V(cos.shape, F32), V(cos.shape, F32), V((rows, D), BF16),
            V(w_query.shape, BF16), V(w_down_kv.shape, BF16), V(w_rope_key.shape[::-1], BF16),
            V(w_up_kv.shape, BF16), V(w_output.shape, BF16),
            V((SP, q, LANE), F32), V((SP, q, LANE), F32), V((q, LANE), F32), V((T, SP, q, LANE), F32),
            V((T, rows, D), BF16), V((T, rows, D), BF16), V((16 if split else crows, D), BF16),
            V((Z, Y, C, T, rows + (32 if split else 16), kvl), BF16), V((Z, Y, C, crp + 16, kvl), BF16),
            V((n, kvl), BF16), V((ROPE, n), F32), V((1, n), F32), V((w_up_kv.shape[2], kvl), BF16),
            V((heads, group, QK), BF16), V((group, heads * HD), BF16),
            V((T - 1, rows, D), BF16), V((T - 1, rows, D), BF16),
            dma((10,)), dma((chunks,)), dma((T - 1,)), dma((T - 1,)), dma((SP - 1,)), dma((SP - 1,)),
            dma((ND - 1,)), dma((ND - 1,)), dma((Z - 1,)), dma((Z - 1,)), dma((Z - 1,)), dma((Z - 1,)),
            dma((1,)), dma((1,)), dma((1,)), dma((1,)), dma((T - 1,)), dma((T - 1,)),
            dma((1,)), dma((1,)), dma((1,)), dma((1,)), dma((T - 1,)), dma((T - 1,)), dma((T - 1,)), dma((T - 1,)),
            dma((chunks, T - 1)), dma((chunks, T - 1)),
        ],
        compiler_params=pltpu.CompilerParams(
            collective_id=0, has_side_effects=True, vmem_limit_bytes=60 * 1024 * 1024),
    )(
        latent_tokens, context_tokens, cond.reshape(SP, prows), ctx_cond.reshape(SP, prows),
        mod_shift, mod_scale, mod_gate, norm_gain.reshape(1, -1), w_query, query_gain.reshape(1, -1),
        w_down_kv, w_rope_key.T, kv_gain.reshape(1, -1), w_up_kv, key_gain.reshape(1, -1), ctx_lift,
        w_output, cos, sin,
    )


def solution(mesh):
    return jax.shard_map(
        local,
        mesh=mesh,
        in_specs=(
            P(("sp", "tp"), None),
            P("sp", None),
            P(),
            P(),
            P("sp", "tp"),
            P("sp", "tp"),
            P("sp", "tp"),
            P(),
            P(None, "tp"),
            P(),
            P(),
            P(),
            P(),
            P(None, None, "tp"),
            P(),
            P("tp"),
            P("tp", None),
        ),
        out_specs=P(("sp", "tp"), None),
        check_vma=False,
    )
```

```python
import functools

import jax
import jax.numpy as jnp
import numpy as np
from jax import lax
from jax.experimental import pallas as pl
from jax.experimental.pallas import tpu as pltpu
from jax.sharding import PartitionSpec as P

HD = 64
ROPE = 32
QK = 96
GRID_W = 64
EPS = 1e-06
THETA = 10000.0
LANE = 128
MESH = pl.DeviceIdType.MESH
F32 = jnp.float32
BF16 = jnp.bfloat16

NN = (((1,), (0,)), ((), ()))
NT = (((1,), (1,)), ((), ()))


def dot(a, b, dims=NN):
    return lax.dot_general(a, b, dims, preferred_element_type=F32)


def column(row):
    return jnp.transpose(jnp.broadcast_to(row, (LANE, row.shape[1])))


def kernel(
    sizes,
    tok_ref, ctx_ref, cond_ref, cctx_ref, mshift_hbm, mscale_hbm, mgate_hbm, ngain_ref,
    wq_hbm, qgain_ref, wd_hbm, wr_hbm, kvgain_ref, wup_hbm, kgain_ref, lift_ref, wo_hbm,
    cos_hbm, sin_hbm,
    out_hbm,
    mshift_ref, mscale_ref, mgate_ref, cos_ref, sin_ref, out_ref,
    wq, wd, wr, wup, wo, part, rsb, red, mod, tokall, hid, chid, G, H, X, rot, ssr, wkT, Q, att,
    sendb, recvb,
    wsem, osem, tok_s, tok_r, rs_s, rs_r, ag_s, ag_r, gz_s, gz_r, hz_s, hz_r, gy_s, gy_r, hy_s, hy_r,
    gx_s, gx_r, rl_s, rl_r, gc_s, gc_r, hc_s, hc_r, f2_s, f2_r, f3_s, f3_r, ob_s, ob_r,
):
    SP, T, Y, C, q, rows, crows, heads, split, chunks = sizes
    Z = SP // (Y * C)
    ND = SP * T
    D = tok_ref.shape[1]
    group = rows * T
    crp = H.shape[3] - 16
    n_ctx = crows * SP
    n_lat = group * SP
    N = n_ctx + n_lat
    sp = lax.axis_index("sp")
    tp = lax.axis_index("tp")
    c = lax.rem(sp, C)
    y = lax.rem(sp // C, Y)
    z = sp // (C * Y)
    flat = sp * T + tp

    barrier = pltpu.get_barrier_semaphore()

    def greet(k, _):
        other = lax.rem(flat + k, ND)
        pl.semaphore_signal(barrier, inc=1, device_id=(other // T, lax.rem(other, T)), device_id_type=MESH)
        return 0

    lax.fori_loop(1, ND, greet, 0)

    wcopies = [
        pltpu.make_async_copy(src, dst, wsem.at[i])
        for i, (src, dst) in enumerate((
            (mshift_hbm, mshift_ref), (mscale_hbm, mscale_ref), (mgate_hbm, mgate_ref), (wd_hbm, wd),
            (wr_hbm, wr), (wup_hbm, wup), (cos_hbm, cos_ref), (sin_hbm, sin_ref), (wq_hbm, wq), (wo_hbm, wo)))
    ]
    for cp in wcopies:
        cp.start()

    sig_l = cond_ref[pl.ds(sp, 1), :]
    sig_l = column(sig_l * jax.nn.sigmoid(sig_l))
    sig_c = cctx_ref[pl.ds(sp, 1), :]
    sig_c = column(sig_c * jax.nn.sigmoid(sig_c))
    pcols = mshift_ref.shape[1] // LANE
    for cp in wcopies[:3]:
        cp.wait()

    def put(v, j, val):
        i = v * pcols + j
        part[i // q, i % q : i % q + 1, :] = val

    for j in range(pcols):
        cols = slice(j * LANE, (j + 1) * LANE)
        w = mshift_ref[:, cols].astype(F32)
        put(0, j, jnp.sum(w * sig_l, axis=0, keepdims=True))
        put(1, j, jnp.sum(w * sig_c, axis=0, keepdims=True))
        w = mscale_ref[:, cols].astype(F32)
        put(2, j, jnp.sum(w * sig_l, axis=0, keepdims=True))
        put(3, j, jnp.sum(w * sig_c, axis=0, keepdims=True))
        w = mgate_ref[:, cols].astype(F32)
        put(4, j, jnp.sum(w * sig_l, axis=0, keepdims=True))
    for i in range(5 * pcols, SP * q):
        part[i // q, i % q : i % q + 1, :] = jnp.zeros((1, LANE), F32)

    pl.semaphore_wait(barrier, ND - 1)

    def rs_copy(k):
        other = lax.rem(sp + k, SP)
        return pltpu.make_async_remote_copy(
            src_ref=part.at[other], dst_ref=rsb.at[sp], send_sem=rs_s.at[k - 1], recv_sem=rs_r.at[k - 1],
            device_id=(other, tp), device_id_type=MESH)

    def rs_start(k, _):
        rs_copy(k).start()
        return 0

    lax.fori_loop(1, SP, rs_start, 0)

    def tp_copy(k, src, dst, s, r):
        return pltpu.make_async_remote_copy(
            src_ref=src, dst_ref=dst, send_sem=s.at[k - 1], recv_sem=r.at[k - 1],
            device_id=(sp, lax.rem(tp + k, T)), device_id_type=MESH)

    tok_copies = [tp_copy(k, tok_ref, tokall.at[tp], tok_s, tok_r) for k in range(1, T)]
    rsb[sp] = part[sp]

    def rs_wait(k, _):
        rs_copy(k).wait()
        return 0

    lax.fori_loop(1, SP, rs_wait, 0)
    total = rsb[0]
    for i in range(1, SP):
        total = total + rsb[i]
    red[...] = total

    def ag_copy(k):
        other = lax.rem(flat + k, ND)
        return pltpu.make_async_remote_copy(
            src_ref=red, dst_ref=mod.at[tp, sp], send_sem=ag_s.at[k - 1], recv_sem=ag_r.at[k - 1],
            device_id=(other // T, lax.rem(other, T)), device_id_type=MESH)

    def ag_start(k, _):
        ag_copy(k).start()
        return 0

    lax.fori_loop(1, ND, ag_start, 0)
    for cp in tok_copies:
        cp.start()
    mod[tp, sp] = total

    for cp in wcopies[3:6]:
        cp.wait()
    wkT[...] = jnp.transpose(wup[0].astype(F32)).astype(BF16)
    kg = column(kgain_ref[...])
    qg = column(qgain_ref[...])
    my_ctx = ctx_ref[pl.ds(pl.multiple_of(tp * 16, 16), 16), :] if split else ctx_ref[...]
    my_ctx = my_ctx.astype(F32)
    invc = lax.rsqrt(jnp.mean(my_ctx * my_ctx, axis=1, keepdims=True) + EPS)
    my_tok = tok_ref[...].astype(F32)
    invt = lax.rsqrt(jnp.mean(my_tok * my_tok, axis=1, keepdims=True) + EPS)

    def ag_wait(k, _):
        ag_copy(k).wait()
        return 0

    lax.fori_loop(1, ND, ag_wait, 0)

    def vec(v, col):
        i = v * pcols + col % pcols
        return mod[col // pcols, i // q, i % q : i % q + 1, :]

    def modulate(x, inv, j, a, b):
        cols = slice(j * LANE, (j + 1) * LANE)
        return (x[:, cols] * inv * ngain_ref[:, cols] * (1.0 + vec(a, j)) + vec(b, j)).astype(BF16)

    for j in range(D // LANE):
        cols = slice(j * LANE, (j + 1) * LANE)
        hid[tp, :, cols] = modulate(my_tok, invt, j, 2, 0)
        chid[:, cols] = modulate(my_ctx, invc, j, 3, 1)

    def squeeze(raw):
        return (raw * lax.rsqrt(jnp.mean(raw * raw, axis=1, keepdims=True) + EPS) * kvgain_ref[...]).astype(BF16)

    lane = lax.broadcasted_iota(jnp.int32, (ROPE, LANE), 1)
    own = hid[tp]
    own_c = chid[...]
    crn = own_c.shape[0]
    lrope = dot(wr[...], jnp.concatenate([own] * T, axis=0), NT)
    crope = dot(wr[...], jnp.concatenate([own_c.astype(F32)] * (LANE // crn), axis=0).astype(BF16), NT)
    llo = tp * rows
    lrope = jnp.where((lane >= llo) & (lane < llo + rows), lrope, 0.0)
    per = (rows if split else LANE) // crn
    clo = lax.rem(sp, per) * crn
    if split:
        clo = clo + lax.rem(tp + 1, T) * rows
    crope = jnp.where((lane >= clo) & (lane < clo + crn), crope, 0.0)
    if split:
        lrope = lrope + crope
        lats = squeeze(dot(jnp.concatenate([own, own_c], axis=0), wd[...]))
        G[z, y, c, tp, rows + 16 : rows + 32] = lats[rows:]
        G[z, y, c, tp, 0:rows] = lats[:rows]
    else:
        H[z, y, c, 0:crows] = squeeze(dot(own_c, wd[...]))
        H[z, y, c, crp : crp + 16] = jnp.concatenate([crope[:16], crope[16:]], axis=1).astype(BF16)
        G[z, y, c, tp, 0:rows] = squeeze(dot(own, wd[...]))
    G[z, y, c, tp, rows : rows + 16] = jnp.concatenate([lrope[:16], lrope[16:]], axis=1).astype(BF16)

    def at(zz, yy, cc):
        return (zz * Y + yy) * C + cc

    def remote(src, s, r, dev):
        return pltpu.make_async_remote_copy(
            src_ref=src, dst_ref=src, send_sem=s, recv_sem=r, device_id=dev, device_id_type=MESH)

    ydev = (at(z, Y - 1 - y, c), tp)
    cdev = (at(z, y, C - 1 - c), tp)

    def xdev(k):
        return (sp, lax.rem(tp + k, T))

    def start(copies):
        for cp in copies:
            cp.start()
        return copies

    def wait(copies):
        for cp in copies:
            cp.wait()

    def finish(sent, got):
        for cp in sent:
            cp.wait_send()
        for cp in got:
            cp.wait_recv()

    zs = [lax.rem(z - k + Z, Z) for k in range(Z)]
    zc, hc = [], []
    for k in range(1, Z):
        dev = (at(lax.rem(z + k, Z), y, c), tp)
        zc.append(remote(G.at[z, y, c, tp], gz_s.at[k - 1], gz_r.at[k - 1], dev))
        if not split:
            hc.append(remote(H.at[z, y, c], hz_s.at[k - 1], hz_r.at[k - 1], dev))
    for cp in zc + hc:
        cp.start()

    def ycol(zz):
        return remote(G.at[zz, y, c, tp], gy_s.at[zz], gy_r.at[zz], ydev)

    def xcol(k, zz):
        return remote(G.at[zz, y, c, tp], gx_s.at[k - 1, zz], gx_r.at[k - 1, zz], xdev(k))

    def got(ref, s, sem):
        return pltpu.make_async_remote_copy(
            src_ref=ref, dst_ref=ref, send_sem=s, recv_sem=sem, device_id=ydev, device_id_type=MESH)

    column_copies = start([ycol(zs[0])] + [xcol(k, zs[0]) for k in range(1, T)])

    for cp in tok_copies:
        cp.wait()
    for k in range(1, T):
        t = lax.rem(tp + k, T)
        x = tokall[t].astype(F32)
        inv = lax.rsqrt(jnp.mean(x * x, axis=1, keepdims=True) + EPS)
        for j in range(D // LANE):
            hid[t, :, j * LANE : (j + 1) * LANE] = modulate(x, inv, j, 2, 0)
    for cp in wcopies[6:9]:
        cp.wait()
    hid_all = hid[...].reshape(group, D)
    raw = dot(hid_all, wq[...])
    rawT = jnp.transpose(raw)
    cosg = cos_ref[:, pl.ds(pl.multiple_of(sp * group, group), group)]
    sing = sin_ref[:, pl.ds(pl.multiple_of(sp * group, group), group)]
    fold = QK ** (-0.5) * 1.4426950408889634
    for h in range(heads):
        u = rawT[h * QK : (h + 1) * QK]
        u = u * (lax.rsqrt(jnp.mean(u * u, axis=0, keepdims=True) + EPS) * fold) * qg[:, :group]
        f, b = u[HD : HD + 16], u[HD + 16 :]
        u = jnp.concatenate([u[:HD], f * cosg - b * sing, b * cosg + f * sing], axis=0)
        Q[h] = jnp.transpose(u).astype(BF16)

    for k in range(1, Z):
        zc[k - 1].wait()
        column_copies += start([ycol(zs[k])] + [xcol(j, zs[k]) for j in range(1, T)])
    for cp in hc:
        cp.wait()

    first = start([remote(G.at[:, y, c, tp], gc_s.at[0], gc_r.at[0], cdev)])
    others = [lax.rem(tp + k, T) for k in range(1, T)]

    def fwd2(cc):
        if cc == 0:
            return [remote(G.at[:, 1 - y, 0, tp], f2_s.at[0], f2_r.at[0], cdev)]
        return [remote(G.at[:, y, 1, t], f2_s.at[k], f2_r.at[k], cdev) for k, t in enumerate(others)]

    def fwd3(cc):
        if cc == 0:
            return [remote(G.at[:, :, 0, t], f3_s.at[k], f3_r.at[k], cdev) for k, t in enumerate(others)]
        return [remote(G.at[:, 1 - y, 1], f3_s.at[0], f3_r.at[0], cdev)]

    def y_in(zz):
        return got(G.at[zz, 1 - y, c, tp], gy_s.at[zz], gy_r.at[zz])

    def x_in(k, zz):
        return got(G.at[zz, y, c, lax.rem(tp - k + T, T)], gx_s.at[k - 1, zz], gx_r.at[k - 1, zz])

    @pl.when(c == 0)
    def _():
        relayed = []
        for zz in zs:
            y_in(zz).wait_recv()
            relayed += start([
                remote(G.at[zz, 1 - y, 0, tp], rl_s.at[k - 1, zz], rl_r.at[k - 1, zz], xdev(k)) for k in range(1, T)])
        sent = start(fwd2(0))
        for zz in zs:
            for k in range(1, T):
                x_in(k, zz).wait_recv()
        wait(relayed)
        finish(sent + start(fwd3(0)), fwd2(1) + fwd3(1))

    @pl.when(c != 0)
    def _():
        relayed = []
        for zz in zs:
            for k in range(1, T):
                x_in(k, zz).wait_recv()
                relayed += start([
                    remote(G.at[zz, y, 1, lax.rem(tp - k + T, T)], rl_s.at[k - 1, zz], rl_r.at[k - 1, zz], ydev)])
        sent = start(fwd2(1))
        for zz in zs:
            y_in(zz).wait_recv()
        wait(relayed)
        finish(sent + start(fwd3(1)), fwd2(0) + fwd3(0))

    for cp in column_copies:
        cp.wait_send()
    wait(first)
    if not split:
        wait(start([remote(H.at[:, y, c], hy_s.at[0], hy_r.at[0], ydev)]))
        wait(start([remote(H.at[:, :, c], hc_s.at[0], hc_r.at[0], cdev)]))

    def where_is(s):
        return s // (Y * C), (s // C) % Y, s % C

    gk = kg[HD:]
    gf, gb = gk[:16], gk[16:]

    def place(cols, total, pos):
        f, b = total[:, :LANE], total[:, LANE:]
        ssr[:, cols] = jnp.sum(f * f + b * b, axis=0, keepdims=True)
        f, b = f * gf, b * gb
        if pos is not None:
            cs, sn = cos_ref[:, pos], sin_ref[:, pos]
            f, b = f * cs - b * sn, b * cs + f * sn
        rot[0:16, cols] = f
        rot[16:32, cols] = b

    lane2 = lax.rem(lax.broadcasted_iota(jnp.int32, (16, 2 * LANE), 1), LANE) // rows

    def mix(blocks):
        total = blocks[0]
        for t in range(1, T):
            total = jnp.where(lane2 == t, blocks[t], total)
        return total

    ctotal = 0.0
    for s in range(SP):
        w = where_is(s)
        lo = n_ctx + s * group
        for t in range(T):
            X[lo + t * rows : lo + (t + 1) * rows] = G[w[0], w[1], w[2], t, 0:rows]
        blocks = [G[w[0], w[1], w[2], t, rows : rows + 16].astype(F32) for t in range(T)]
        place(slice(lo, lo + group), mix(blocks), slice(s * group, (s + 1) * group))
        if split:
            base = s // per * group
            for t in range(T):
                lo = base + (t + 1) % T * rows + s % per * 16
                X[lo : lo + 16] = G[w[0], w[1], w[2], t, rows + 16 : rows + 32]
            ctotal = ctotal + mix([blocks[(t - 1) % T] for t in range(T)])
            if s % per == per - 1:
                place(slice(base, base + group), ctotal, None)
                ctotal = 0.0
    if not split:
        if crows % 16 == 0:
            for s in range(SP):
                w = where_is(s)
                X[s * crows : (s + 1) * crows] = H[w[0], w[1], w[2], 0:crows]
        else:
            X[0:n_ctx] = jnp.concatenate(
                [H[where_is(s)][0:16].astype(F32)[:crows] for s in range(SP)], axis=0).astype(BF16)
        for s0 in range(0, SP, per):
            total = sum(H[where_is(s)][crp : crp + 16].astype(F32) for s in range(s0, s0 + per))
            place(slice(s0 * crows, s0 * crows + LANE), total, None)

    gp = kg[:HD, :1]
    ones = jnp.ones((N, LANE), BF16)
    half = lax.broadcasted_iota(jnp.int32, (group, LANE), 1) < HD

    def pair(p, _):
        lo = pl.multiple_of(p * LANE, LANE)
        kT = dot(wkT[pl.ds(lo, LANE), :], X[...], NT)
        val = jnp.concatenate([dot(X[...], wup[1, :, pl.ds(lo, LANE)]).astype(BF16), ones], axis=1)
        res = []
        for i in range(2):
            kp = kT[i * HD : (i + 1) * HD]
            inv = lax.rsqrt((jnp.sum(kp * kp, axis=0, keepdims=True) + ssr[...]) * (1.0 / QK) + EPS)
            key = jnp.concatenate([kp * gp * inv, rot[...] * inv], axis=0).astype(BF16)
            w = jnp.exp2(dot(Q[2 * p + i], key)).astype(BF16)
            drop = jnp.exp(jnp.full((1, 2 * LANE), -lift_ref[2 * p + i], F32))
            o = dot(w[:, :n_ctx], val[:n_ctx]) + drop * dot(w[:, n_ctx:], val[n_ctx:])
            res.append(o[:, :LANE] / o[:, LANE:])
        att[:, pl.ds(lo, LANE)] = jnp.where(half, res[0], res[1]).astype(BF16)
        return 0

    lax.fori_loop(0, heads // 2, pair, 0)

    wcopies[9].wait()
    width = D // chunks
    copies = []
    for j in range(chunks):
        cols = slice(j * width, (j + 1) * width)
        for k in range(1, T):
            t = lax.rem(tp + k, T)
            a = att[pl.ds(pl.multiple_of(t * rows, rows), rows), :]
            sendb[k - 1, :, cols] = dot(a, wo[:, cols]).astype(BF16)
            cp = pltpu.make_async_remote_copy(
                src_ref=sendb.at[k - 1, :, cols], dst_ref=recvb.at[k - 1, :, cols],
                send_sem=ob_s.at[j, k - 1], recv_sem=ob_r.at[j, k - 1],
                device_id=xdev(k), device_id_type=MESH)
            cp.start()
            copies.append(cp)
    acc = dot(att[pl.ds(pl.multiple_of(tp * rows, rows), rows), :], wo[...])
    outs = []
    for j in range(chunks):
        for k in range(1, T):
            copies[j * (T - 1) + k - 1].wait()
        for i in range(j * width // LANE, (j + 1) * width // LANE):
            cols = slice(i * LANE, (i + 1) * LANE)
            o = acc[:, cols]
            for k in range(1, T):
                o = o + recvb[k - 1, :, cols].astype(F32)
            out_ref[:, cols] = (tok_ref[:, cols].astype(F32) + vec(4, i) * o).astype(BF16)
        cols = slice(j * width, (j + 1) * width)
        cp = pltpu.make_async_copy(out_ref.at[:, cols], out_hbm.at[:, cols], osem.at[j])
        cp.start()
        outs.append(cp)
    for cp in outs:
        cp.wait()


def local(
    latent_tokens, context_tokens, cond, ctx_cond, mod_shift, mod_scale, mod_gate, norm_gain,
    w_query, query_gain, w_down_kv, w_rope_key, kv_gain, w_up_kv, key_gain, ctx_lift, w_output,
):
    SP, T = lax.axis_size("sp"), lax.axis_size("tp")
    Y = C = 2
    Z = SP // (Y * C)
    rows, D = latent_tokens.shape
    crows = context_tokens.shape[0]
    heads = ctx_lift.shape[0]
    prows, pcols = mod_shift.shape
    kvl = w_down_kv.shape[1]
    q = -(-(5 * pcols // LANE) // SP)
    group = rows * T
    seq = group * SP
    n = seq + crows * SP
    split = crows == 16 * T
    crp = 16 if split else max(16, crows)
    chunks = 4
    inv = THETA ** (-np.arange(ROPE // 4, dtype=np.float64) / (ROPE // 4))
    pos = np.arange(seq)
    ang = np.concatenate([inv[:, None] * (pos // GRID_W), inv[:, None] * (pos % GRID_W)], axis=0)
    cos, sin = np.cos(ang).astype(np.float32), np.sin(ang).astype(np.float32)
    vm = pl.BlockSpec(memory_space=pltpu.VMEM)
    hbm = pl.BlockSpec(memory_space=pl.ANY)
    sm = pl.BlockSpec(memory_space=pltpu.SMEM)
    dma = pltpu.SemaphoreType.DMA
    V = pltpu.VMEM
    ND = SP * T
    return pl.pallas_call(
        functools.partial(kernel, (SP, T, Y, C, q, rows, crows, heads, split, chunks)),
        out_shape=jax.ShapeDtypeStruct((rows, D), BF16),
        in_specs=[vm] * 4 + [hbm] * 3 + [vm, hbm, vm, hbm, hbm, vm, hbm, vm, sm, hbm, hbm, hbm],
        out_specs=hbm,
        scratch_shapes=[
            V(mod_shift.shape, BF16), V(mod_shift.shape, BF16), V(mod_shift.shape, BF16),
            V(cos.shape, F32), V(cos.shape, F32), V((rows, D), BF16),
            V(w_query.shape, BF16), V(w_down_kv.shape, BF16), V(w_rope_key.shape[::-1], BF16),
            V(w_up_kv.shape, BF16), V(w_output.shape, BF16),
            V((SP, q, LANE), F32), V((SP, q, LANE), F32), V((q, LANE), F32), V((T, SP, q, LANE), F32),
            V((T, rows, D), BF16), V((T, rows, D), BF16), V((16 if split else crows, D), BF16),
            V((Z, Y, C, T, rows + (32 if split else 16), kvl), BF16), V((Z, Y, C, crp + 16, kvl), BF16),
            V((n, kvl), BF16), V((ROPE, n), F32), V((1, n), F32), V((w_up_kv.shape[2], kvl), BF16),
            V((heads, group, QK), BF16), V((group, heads * HD), BF16),
            V((T - 1, rows, D), BF16), V((T - 1, rows, D), BF16),
            dma((10,)), dma((chunks,)), dma((T - 1,)), dma((T - 1,)), dma((SP - 1,)), dma((SP - 1,)),
            dma((ND - 1,)), dma((ND - 1,)), dma((Z - 1,)), dma((Z - 1,)), dma((Z - 1,)), dma((Z - 1,)),
            dma((Z,)), dma((Z,)), dma((1,)), dma((1,)), dma((T - 1, Z)), dma((T - 1, Z)), dma((T - 1, Z)), dma((T - 1, Z)),
            dma((1,)), dma((1,)), dma((1,)), dma((1,)), dma((T - 1,)), dma((T - 1,)), dma((T - 1,)), dma((T - 1,)),
            dma((chunks, T - 1)), dma((chunks, T - 1)),
        ],
        compiler_params=pltpu.CompilerParams(
            collective_id=0, has_side_effects=True, vmem_limit_bytes=60 * 1024 * 1024),
    )(
        latent_tokens, context_tokens, cond.reshape(SP, prows), ctx_cond.reshape(SP, prows),
        mod_shift, mod_scale, mod_gate, norm_gain.reshape(1, -1), w_query, query_gain.reshape(1, -1),
        w_down_kv, w_rope_key.T, kv_gain.reshape(1, -1), w_up_kv, key_gain.reshape(1, -1), ctx_lift,
        w_output, cos, sin,
    )


def solution(mesh):
    return jax.shard_map(
        local,
        mesh=mesh,
        in_specs=(
            P(("sp", "tp"), None),
            P("sp", None),
            P(),
            P(),
            P("sp", "tp"),
            P("sp", "tp"),
            P("sp", "tp"),
            P(),
            P(None, "tp"),
            P(),
            P(),
            P(),
            P(),
            P(None, None, "tp"),
            P(),
            P("tp"),
            P("tp", None),
        ),
        out_specs=P(("sp", "tp"), None),
        check_vma=False,
    )
```
